32 devices in a mesh: sp: 16 (over z, y, x), tp: 2 (over core).
Axes of the slice: x: 2, y: 2, z: 4, core: 2. Of those that a mesh axis runs over, the one named last changes fastest.
Arguments:
- tokens: bfloat16 [4096, 2048], P('sp'), may hold values from -6 to 6
- input_norm_gain: float32 [2048], replicated, may hold values from 0.1 to 1.9
- query_matrix: bfloat16 [2048, 1024], P('sp', 'tp'), may hold values from -0.125 to 0.125
- key_matrix: bfloat16 [2048, 1024], P('sp', 'tp'), may hold values from -0.125 to 0.125
- value_matrix: bfloat16 [2048, 1024], P('sp', 'tp'), may hold values from -0.125 to 0.125
- convolution_value_matrix: bfloat16 [2048, 2048], P('sp', 'tp'), may hold values from -0.125 to 0.125
- convolution_gate_matrix: bfloat16 [2048, 2048], P('sp', 'tp'), may hold values from -0.125 to 0.125
- decay_offset_channel: float32 [1024], P('tp'), may hold values from -16 to -2
- decay_first_matrix: bfloat16 [2048, 128], replicated, may hold values from -0.125 to 0.125
- decay_second_matrix: bfloat16 [128, 1024], P(None, 'tp'), may hold values from -0.59765625 to 0.59765625
- learning_rate_offset: float32 [1024], P('tp'), may hold values from -9 to 1
- learning_rate_first_matrix: bfloat16 [2048, 128], replicated, may hold values from -0.125 to 0.125
- learning_rate_second_matrix: bfloat16 [128, 1024], P(None, 'tp'), may hold values from -0.5 to 0.5
- forgetting_rate_factor: float32 [4096, 16], P('sp', 'tp'), may hold values from 0.39 to 2.53
- state_retention_share: float32 [4096, 16], P('sp', 'tp'), may hold values from 0.12 to 1
- per_head_norm_gain: float32 [1024], P('tp'), may hold values from 0.1 to 1.9
- convolution_filter_taps: float32 [31, 2048], P(None, 'tp'), may hold values from -81 to 81
- convolution_channel_gain: float32 [2048], P('tp'), may hold values from 0.1 to 1.9
- attention_output_matrix: bfloat16 [2048, 1024], P('sp', 'tp'), may hold values from -0.109375 to 0.109375
- convolution_output_matrix: bfloat16 [2048, 2048], P('sp', 'tp'), may hold values from -0.109375 to 0.109375
Outputs:
- mixed: bfloat16 [4096, 2048], P('sp')
The draws below stay inside these ranges and needn't reach their ends.
All inputs are finite; a program needn't handle non-finite values.
Results may differ from the reference program's by a relative error of at most 0.014.
Values may be sent and summed in bfloat16 or wider, within the bound.
A program may use at most 128 MiB of HBM per device.

```python
import jax
import jax.numpy as jnp
from jax import lax

D = 2048
RHEADS = 16
HEAD = 64
RW = 1024
CONV_CH = 2048
CONV_SPAN = 31
LOWRANK = 128
TOK_DEV = 256
TOKENS = 4096
N_TP = 2


def rate_levels(key):
    order = jax.random.permutation(jax.random.fold_in(key, 11), RHEADS)
    fast_count = RHEADS // 2
    fast = jnp.repeat(order < fast_count, HEAD)
    spread = jax.random.uniform(jax.random.fold_in(key, 12), (RW,), jnp.float32)
    other = jax.random.uniform(jax.random.fold_in(key, 13), (RW,), jnp.float32)
    fast_log = jnp.log(1.0 / 60.0) + spread * jnp.log(3.0)
    slow_log = jnp.log(0.01 / TOKENS) + spread * jnp.log(5.0)
    decay_level = jnp.where(fast, fast_log, slow_log) + 0.5
    rate_level = jnp.where(fast, 2.0 * other - 1.0, jnp.log(10.0 / TOKENS) + other - 0.5)
    return (decay_level, rate_level)


def draw_decay_offset_channel(key, part):
    return rate_levels(key)[0]


def draw_learning_rate_offset(key, part):
    return rate_levels(key)[1]


def draw_forgetting_rate_factor(key, part):
    spans = TOKENS // TOK_DEV
    level = jnp.exp(jax.random.uniform(jax.random.fold_in(key, 21), (spans, RHEADS), jnp.float32, -0.7, 0.7))
    rough = jax.random.uniform(jax.random.fold_in(key, 22), (TOKENS, RHEADS), jnp.float32, 0.8, 1.25)
    return jnp.repeat(level, TOK_DEV, axis=0) * rough


def draw_state_retention_share(key, part):
    places = jax.random.randint(jax.random.fold_in(key, 31), (3, RHEADS), 0, TOKENS)
    depth = jax.random.uniform(jax.random.fold_in(key, 32), (3, RHEADS), jnp.float32, 0.6, 0.8)
    struck = jnp.arange(TOKENS, dtype=jnp.int32)[:, None, None] == places[None]
    return jnp.prod(jnp.where(struck, depth[None], 1.0), axis=1)


def draw_convolution_filter_taps(key, part):
    taps = jnp.exp(jax.random.uniform(jax.random.fold_in(key, 41), (CONV_SPAN, 1), jnp.float32, 0.0, jnp.log(10.0)))
    place = jnp.arange(CONV_CH, dtype=jnp.float32)[None, :] / CONV_CH
    rising = jnp.exp(place * jnp.log(10.0))
    rough = jax.random.uniform(jax.random.fold_in(key, 42), (1, CONV_CH), jnp.float32, 0.5, 1.5)
    base = jax.random.truncated_normal(jax.random.fold_in(key, 43), -4.0, 4.0, (CONV_SPAN, CONV_CH), jnp.float32)
    return base * taps * rising * rough / (4.0 * CONV_SPAN ** 0.5)


def block_scale(key, dims, shards, smallest, largest):
    def one(dim, blocks):
        draws = jax.random.uniform(jax.random.fold_in(jax.random.fold_in(key, 6), dim), (blocks,), jnp.float32, smallest / len(shards), largest / len(shards))
        return jnp.repeat(jnp.exp(draws), dims[dim] // blocks).reshape((-1,) + (1,) * (len(dims) - dim - 1))

    loudness = one(*shards[0])
    for cut in shards[1:]:
        loudness = loudness * one(*cut)
    return loudness


def bell_draw(stream_key, extent, width, bound, split=(), kind=jnp.bfloat16):
    entries = jax.random.normal(stream_key, extent, jnp.float32) * width
    if len(split) > 0:
        entries = block_scale(stream_key, extent, split, -0.22, 0.18) * entries
    return jnp.clip(entries, min=-bound, max=bound).astype(kind)


def setup_inputs(seed: int = 0) -> dict:
    arg_keys = jax.random.split(jax.random.key(seed), 21)
    return {
        "tokens": bell_draw(arg_keys[0], (TOKENS, D), 1.0, 6.0, ((0, 16),)),
        "input_norm_gain": jnp.clip(1.0 + 0.18 * jax.random.normal(arg_keys[1], (D,), jnp.float32), 0.1, 1.9),
        "query_matrix": bell_draw(arg_keys[2], (D, RW), D ** -0.5, 0.125, ((0, 16), (1, 2))),
        "key_matrix": bell_draw(arg_keys[3], (D, RW), D ** -0.5, 0.125, ((0, 16), (1, 2))),
        "value_matrix": bell_draw(arg_keys[4], (D, RW), D ** -0.5, 0.125, ((0, 16), (1, 2))),
        "convolution_value_matrix": bell_draw(arg_keys[5], (D, CONV_CH), D ** -0.5, 0.125, ((0, 16), (1, 2))),
        "convolution_gate_matrix": bell_draw(arg_keys[6], (D, CONV_CH), D ** -0.5, 0.125, ((0, 16), (1, 2))),
        "decay_offset_channel": draw_decay_offset_channel(jax.random.fold_in(arg_keys[20], 71), 0),
        "decay_first_matrix": bell_draw(arg_keys[8], (D, LOWRANK), D ** -0.5, 0.125),
        "decay_second_matrix": bell_draw(arg_keys[9], (LOWRANK, RW), 0.1, 0.59765625, ((1, 2),)),
        "learning_rate_offset": draw_learning_rate_offset(jax.random.fold_in(arg_keys[20], 71), 0),
        "learning_rate_first_matrix": bell_draw(arg_keys[11], (D, LOWRANK), D ** -0.5, 0.125),
        "learning_rate_second_matrix": bell_draw(arg_keys[12], (LOWRANK, RW), LOWRANK ** -0.5, 0.5, ((1, 2),)),
        "forgetting_rate_factor": draw_forgetting_rate_factor(jax.random.fold_in(arg_keys[20], 71), 0),
        "state_retention_share": draw_state_retention_share(jax.random.fold_in(arg_keys[20], 71), 0),
        "per_head_norm_gain": jnp.clip(1.0 + 0.18 * jax.random.normal(arg_keys[15], (RW,), jnp.float32), 0.1, 1.9),
        "convolution_filter_taps": draw_convolution_filter_taps(jax.random.fold_in(arg_keys[20], 71), 0),
        "convolution_channel_gain": jnp.clip(1.0 + 0.18 * jax.random.normal(arg_keys[17], (CONV_CH,), jnp.float32), 0.1, 1.9),
        "attention_output_matrix": bell_draw(arg_keys[18], (D, RW), (RW + CONV_CH) ** -0.5, 0.109375, ((0, 16), (1, 2))),
        "convolution_output_matrix": bell_draw(arg_keys[19], (D, CONV_CH), (RW + CONV_CH) ** -0.5, 0.109375, ((0, 16), (1, 2))),
    }


HIGHEST = lax.Precision.HIGHEST

def reference(tokens, input_norm_gain, query_matrix, key_matrix, value_matrix, convolution_value_matrix, convolution_gate_matrix, decay_offset_channel, decay_first_matrix, decay_second_matrix, learning_rate_offset, learning_rate_first_matrix, learning_rate_second_matrix, forgetting_rate_factor, state_retention_share, per_head_norm_gain, convolution_filter_taps, convolution_channel_gain, attention_output_matrix, convolution_output_matrix):
    widened = tokens.astype(jnp.float32)
    normed = (widened * lax.rsqrt(lax.optimization_barrier(jnp.mean(widened * widened, axis=-1, keepdims=True)) + 1e-06) * input_norm_gain).astype(jnp.bfloat16)
    query_proj = jnp.dot(normed, query_matrix, preferred_element_type=jnp.float32)
    key_proj = jnp.dot(normed, key_matrix, preferred_element_type=jnp.float32)
    value_proj = jnp.dot(normed, value_matrix, preferred_element_type=jnp.float32)
    conv_value = jnp.dot(normed, convolution_value_matrix, preferred_element_type=jnp.float32)
    conv_gate = jnp.dot(normed, convolution_gate_matrix, preferred_element_type=jnp.float32)
    decay_mid = jnp.tanh(jnp.dot(normed, decay_first_matrix, preferred_element_type=jnp.float32)).astype(jnp.bfloat16)
    rate_mid = jnp.dot(normed, learning_rate_first_matrix, preferred_element_type=jnp.float32).astype(jnp.bfloat16)
    logarithm_learning_rate = -jax.nn.softplus(-(decay_offset_channel + jnp.dot(decay_mid, decay_second_matrix, preferred_element_type=jnp.float32))) - 0.5
    learn_rate = jax.nn.sigmoid(learning_rate_offset + jnp.dot(rate_mid, learning_rate_second_matrix, preferred_element_type=jnp.float32))
    reshaped_tensor = (TOKENS, RHEADS, HEAD)
    position_decay_factor = jnp.exp(-jnp.exp(logarithm_learning_rate).reshape(reshaped_tensor) * forgetting_rate_factor[:, :, None]) * state_retention_share[:, :, None]
    key_heads = key_proj.reshape(reshaped_tensor)
    unit_key = key_heads * lax.rsqrt(lax.optimization_barrier(jnp.sum(key_heads * key_heads, axis=-1, keepdims=True)) + 1e-06)
    erase = -unit_key
    write = unit_key * learn_rate.reshape(reshaped_tensor)

    def advance(state, inputs):
        query_t, decay_t, key_t, value_t, erase_t, write_t = inputs
        pulled = jnp.einsum('hvk,hk->hv', state, erase_t, precision=HIGHEST)
        state = state * decay_t[:, None, :] + pulled[:, :, None] * write_t[:, None, :] + value_t[:, :, None] * key_t[:, None, :]
        return (state, jnp.einsum('hvk,hk->hv', state, query_t, precision=HIGHEST))
    final_state, state_rows = lax.scan(advance, jnp.zeros((RHEADS, HEAD, HEAD), jnp.float32), (query_proj.reshape(reshaped_tensor), position_decay_factor, key_heads, value_proj.reshape(reshaped_tensor), erase, write))
    centred = state_rows - lax.optimization_barrier(jnp.mean(state_rows, axis=-1, keepdims=True))
    normal_state = centred * lax.rsqrt(lax.optimization_barrier(jnp.mean(centred * centred, axis=-1, keepdims=True)) + 0.00064)
    state_mixed = (normal_state * per_head_norm_gain.reshape(RHEADS, HEAD)).reshape(TOKENS, RW).astype(jnp.bfloat16)
    gated = (conv_value * jax.nn.sigmoid(conv_gate)).astype(jnp.bfloat16)
    padded = jnp.concatenate([jnp.zeros((CONV_SPAN - 1, CONV_CH), jnp.bfloat16), gated], axis=0)
    filtered = jnp.zeros((TOKENS, CONV_CH), jnp.float32)
    for offset in range(CONV_SPAN):
        filtered = filtered + convolution_filter_taps[offset] * padded[offset:offset + TOKENS].astype(jnp.float32)
    row_mean = lax.optimization_barrier(jnp.mean(filtered, axis=-1, keepdims=True))
    deviation = filtered - row_mean
    variance = lax.optimization_barrier(jnp.mean(deviation * deviation, axis=-1, keepdims=True))
    conv_mixed = jax.nn.silu(deviation * lax.rsqrt(variance + 1e-05) * convolution_channel_gain).astype(jnp.bfloat16)
    state_part = RW // N_TP
    conv_part = CONV_CH // N_TP
    total = jnp.zeros((TOKENS, D), jnp.float32)
    for member in range(N_TP):
        state_lo = member * state_part
        conv_lo = member * conv_part
        partial_value = jnp.dot(state_mixed[:, state_lo:state_lo + state_part], attention_output_matrix[:, state_lo:state_lo + state_part].T, preferred_element_type=jnp.float32)
        partial_value = partial_value + jnp.dot(conv_mixed[:, conv_lo:conv_lo + conv_part], convolution_output_matrix[:, conv_lo:conv_lo + conv_part].T, preferred_element_type=jnp.float32)
        total = total + lax.optimization_barrier(partial_value.astype(jnp.bfloat16)).astype(jnp.float32)
    return total.astype(jnp.bfloat16)
```

```python
import functools
import math

import jax
import jax.numpy as jnp
from jax import lax
from jax.experimental import pallas as pl
from jax.experimental.pallas import tpu as pltpu
from jax.sharding import PartitionSpec as P


HIGHEST = lax.Precision.HIGHEST
RMS_EPSILON = 1e-06
GROUP_EPSILON = 0.00064
LAYER_EPSILON = 1e-05
UNIT_EPSILON = 1e-06
EXP_HALF = math.exp(-0.5)


def split(x):
    top = x.astype(jnp.bfloat16)
    return top, (x - top.astype(jnp.float32)).astype(jnp.bfloat16)


def dot3(left, right, dims=((1,), (0,))):
    (lh, ll), (rh, rl) = split(left), split(right)

    def one(p, q):
        return lax.dot_general(p, q, (dims, ((), ())), preferred_element_type=jnp.float32)

    return one(lh, rh) + (one(lh, rl) + one(ll, rh))


def dot3t(left, right):
    return dot3(left, right, ((1,), (1,)))


def exact(left, right):
    return jnp.dot(left, right, precision=HIGHEST, preferred_element_type=jnp.float32)


def column(values, index):
    lanes = lax.broadcasted_iota(jnp.int32, values.shape, 1)
    return jnp.sum(jnp.where(lanes == index, values, 0.0), axis=1, keepdims=True)


def delta_kernel(
    head_size, chunk, block,
    query_ref, key_ref, value_ref, decay_ref, rate_ref, factor_ref, share_ref,
    local_ref, carried_ref, pair_ref,
):
    rows, width = query_ref.shape
    pair = pl.program_id(0)
    per = width // head_size
    lane = lax.broadcasted_iota(jnp.int32, (1, width), 1)
    lane_head = lane // head_size
    row_w = lax.broadcasted_iota(jnp.int32, (width, width), 0)
    col_w = lax.broadcasted_iota(jnp.int32, (width, width), 1)
    same_head = (row_w // head_size) == (col_w // head_size)
    ones_head = jnp.where(same_head, 1.0, 0.0)
    row_b = lax.broadcasted_iota(jnp.int32, (block, block), 0)
    col_b = lax.broadcasted_iota(jnp.int32, (block, block), 1)
    same_chunk = (row_b // chunk) == (col_b // chunk)
    strict = same_chunk & (row_b > col_b)
    incl = same_chunk & (row_b >= col_b)
    sums = jnp.concatenate([jnp.where(incl, 1.0, 0.0), jnp.where(same_chunk, 1.0, 0.0)], axis=0)
    eye_b = jnp.where(row_b == col_b, 1.0, 0.0)

    factor, share = factor_ref[...], jnp.log(share_ref[...])
    factor_w = jnp.zeros((rows, width), jnp.float32)
    share_w = jnp.zeros((rows, width), jnp.float32)
    for h in range(per):
        factor_w = jnp.where(lane_head == h, column(factor, pair * per + h), factor_w)
        share_w = jnp.where(lane_head == h, column(share, pair * per + h), share_w)
    logdec = share_w - (EXP_HALF * jax.nn.sigmoid(decay_ref[...])) * factor_w
    learn = jax.nn.sigmoid(rate_ref[...])
    key = key_ref[...]
    unit = key * lax.rsqrt(exact(key * key, ones_head) + UNIT_EPSILON)

    blocks = []
    for start in range(0, rows, block):
        cut = slice(start, start + block)
        q, k, v, ld = query_ref[cut], key[cut], value_ref[cut], logdec[cut]
        er, wr = -unit[cut], unit[cut] * learn[cut]
        both = exact(sums, ld)
        gain, total = both[:block], both[block:]
        mid = 0.5 * total
        up, down, bup = jnp.exp(gain - mid), jnp.exp(mid - gain), jnp.exp(gain - ld - mid)
        ehat, qhat, what, khat = er * bup, q * up, wr * down, k * down
        right = jnp.concatenate([what, khat], axis=0)
        eh_full, q_full = er * jnp.exp(gain - ld), q * jnp.exp(gain)
        to_end = jnp.exp(total - gain)
        pulled = solved = local = query = None
        heads = []
        for h in range(per):
            left = jnp.where(lane_head == h, jnp.concatenate([ehat, qhat], axis=0), 0.0)
            grid = dot3t(left, right)
            ew = jnp.where(strict, grid[:block, :block], 0.0)
            ek = jnp.where(strict, grid[:block, block:], 0.0)
            rw = jnp.where(incl, grid[block:, :block], 0.0)
            rk = jnp.where(incl, grid[block:, block:], 0.0)
            size = 2
            off = (row_b // size == col_b // size) & (row_b > col_b)
            inv = eye_b + jnp.where(off, ew, 0.0)
            while size < chunk:
                off = (row_b // (2 * size) == col_b // (2 * size)) & (row_b // size > col_b // size)
                inv = inv + dot3(dot3(inv, jnp.where(off, ew, 0.0)), inv)
                size *= 2
            seen = dot3(jnp.concatenate([ek, rk], axis=0), v)
            both = dot3(inv, jnp.concatenate([seen[:block], eh_full], axis=1))
            read = dot3(rw, both)
            heads.append((both[:, :width], both[:, width:], read[:, :width] + seen[block:], read[:, width:]))
        merged = list(heads[0])
        for h in range(1, per):
            merged = [jnp.where(lane_head == h, new, old) for new, old in zip(heads[h], merged)]
        pulled, solved, local, query = merged
        blocks.append((pulled, solved, local, q_full + query, v, wr * to_end, k * to_end, jnp.exp(total)))

    state = jnp.concatenate([jnp.where(row_w == col_w, 1.0, 0.0), jnp.zeros((width, width), jnp.float32)], axis=0)
    across = ((0,), (0,))
    for number, (pulled, solved, local, query, v, wend, kend, gain) in enumerate(blocks):
        for first in range(0, block, chunk):
            cut = slice(first, first + chunk)
            place = slice(number * block + first, number * block + first + chunk)
            got = dot3t(query[cut], state)
            carried_ref[place] = got[:, :width]
            local_ref[place] = local[cut] + got[:, width:]
            step = jnp.where(same_head, dot3(solved[cut], wend[cut], across), 0.0)
            added = dot3(
                jnp.concatenate([pulled[cut], v[cut]], axis=0),
                jnp.concatenate([wend[cut], kend[cut]], axis=0),
                across,
            )
            added = jnp.where(same_head, added, 0.0)
            moved = state * gain[first : first + 1] + dot3(state, step)
            state = jnp.concatenate([moved[:width], moved[width:] + added], axis=0)
    pair_ref[0] = state


def finish_kernel(head_size, local_ref, carried_ref, state_ref, gain_ref, out_ref):
    width = local_ref.shape[1]
    row_w = lax.broadcasted_iota(jnp.int32, (width, width), 0)
    col_w = lax.broadcasted_iota(jnp.int32, (width, width), 1)
    same_head = (row_w // head_size) == (col_w // head_size)
    average = jnp.where(same_head, 1.0 / head_size, 0.0)
    y = local_ref[...] + dot3t(carried_ref[...], state_ref[0])
    centred = y - exact(y, average)
    variance = exact(centred * centred, average)
    out_ref[...] = (centred * lax.rsqrt(variance + GROUP_EPSILON) * gain_ref[...]).astype(jnp.bfloat16)


def from_behind(value, axis, steps):
    count = lax.axis_size(axis)
    initial, last = (max(0, -steps), min(count, count - steps))
    return lax.ppermute(value, axis, [(source, source + steps) for source in range(initial, last)])


def head_blocks(pairs, head_size):
    width = pairs.shape[-1]
    return jnp.stack(
        [pairs[:, a : a + head_size, a : a + head_size] for a in range(0, width, head_size)], axis=1
    )


def delta_rule(query, key, value, decay_pre, rate_pre, factor, share, gain):
    rows, channels = query.shape
    heads = factor.shape[1]
    head_size = channels // heads
    per = math.gcd(heads, max(1, 128 // head_size))
    width, pairs = per * head_size, heads // per
    block = math.gcd(rows, 128)
    chunk = math.gcd(block, 16)
    wide = pl.BlockSpec((rows, width), lambda i: (0, i))
    whole = pl.BlockSpec((rows, heads), lambda i: (0, 0))
    local, carried, pair = pl.pallas_call(
        functools.partial(delta_kernel, head_size, chunk, block),
        grid=(pairs,),
        in_specs=[wide] * 5 + [whole] * 2,
        out_specs=[wide, wide, pl.BlockSpec((1, 2 * width, width), lambda i: (i, 0, 0))],
        out_shape=[
            jax.ShapeDtypeStruct((rows, channels), jnp.float32),
            jax.ShapeDtypeStruct((rows, channels), jnp.float32),
            jax.ShapeDtypeStruct((pairs, 2 * width, width), jnp.float32),
        ],
        cost_estimate=pl.CostEstimate(
            flops=pairs * rows * width * width * 60, bytes_accessed=rows * channels * 32, transcendentals=rows * channels * 10
        ),
        name="delta_chunks",
    )(query, key, value, decay_pre, rate_pre, factor, share)

    phi, psi = head_blocks(pair[:, :width], head_size), head_blocks(pair[:, width:], head_size)
    both = jnp.concatenate([phi, psi], axis=-2).reshape(heads, 2 * head_size, head_size)
    count, place = lax.axis_size("sp"), lax.axis_index("sp")
    steps = 1
    while steps < count - 1:
        earlier = from_behind(both, "sp", steps)
        new = exact_mul("hcd,hde->hce", earlier, both[:, :head_size])
        new = new + jnp.concatenate([jnp.zeros_like(both[:, :head_size]), both[:, head_size:]], axis=1)
        both = jnp.where(place >= steps, new, both)
        steps *= 2
    state = from_behind(both[:, head_size:], "sp", 1).reshape(pairs, per, head_size, head_size)
    same = jnp.eye(per, dtype=jnp.float32)
    state = (state[:, :, :, None, :] * same[None, :, None, :, None]).reshape(pairs, width, width)
    return pl.pallas_call(
        functools.partial(finish_kernel, head_size),
        grid=(pairs,),
        in_specs=[wide, wide, pl.BlockSpec((1, width, width), lambda i: (i, 0, 0)), pl.BlockSpec((1, width), lambda i: (0, i))],
        out_specs=wide,
        out_shape=jax.ShapeDtypeStruct((rows, channels), jnp.bfloat16),
        name="delta_finish",
    )(local, carried, state, gain[None])


def exact_mul(form, left, right):
    return jnp.einsum(form, left, right, precision=HIGHEST)


def body(
    tokens,
    input_norm_gain,
    query_matrix,
    key_matrix,
    value_matrix,
    convolution_value_matrix,
    convolution_gate_matrix,
    decay_offset_channel,
    decay_first_matrix,
    decay_second_matrix,
    learning_rate_offset,
    learning_rate_first_matrix,
    learning_rate_second_matrix,
    forgetting_rate_factor,
    state_retention_share,
    per_head_norm_gain,
    convolution_filter_taps,
    convolution_channel_gain,
    attention_output_matrix,
    convolution_output_matrix,
):
    tok_rows = tokens.shape[0]
    widened = tokens.astype(jnp.float32)
    normed = (
        widened
        * lax.rsqrt(jnp.mean(widened * widened, axis=-1, keepdims=True) + RMS_EPSILON)
        * input_norm_gain
    ).astype(jnp.bfloat16)
    pieces = (
        lax.all_gather(query_matrix, "sp", axis=0, tiled=True),
        lax.all_gather(key_matrix, "sp", axis=0, tiled=True),
        lax.all_gather(value_matrix, "sp", axis=0, tiled=True),
        lax.all_gather(convolution_value_matrix, "sp", axis=0, tiled=True),
        lax.all_gather(convolution_gate_matrix, "sp", axis=0, tiled=True),
    )
    query_proj, key_proj, value_proj, conv_value, conv_gate = tuple(
        (jnp.dot(normed, piece, preferred_element_type=jnp.float32) for piece in pieces)
    )
    decay_mid = jnp.tanh(
        jnp.dot(normed, decay_first_matrix, preferred_element_type=jnp.float32)
    ).astype(jnp.bfloat16)
    rate_mid = jnp.dot(
        normed, learning_rate_first_matrix, preferred_element_type=jnp.float32
    ).astype(jnp.bfloat16)
    decay_pre = decay_offset_channel + jnp.dot(
        decay_mid, decay_second_matrix, preferred_element_type=jnp.float32
    )
    rate_pre = learning_rate_offset + jnp.dot(
        rate_mid, learning_rate_second_matrix, preferred_element_type=jnp.float32
    )
    state_mixed = delta_rule(
        query_proj, key_proj, value_proj, decay_pre, rate_pre,
        forgetting_rate_factor, state_retention_share, per_head_norm_gain,
    )
    gated = (conv_value * jax.nn.sigmoid(conv_gate)).astype(jnp.bfloat16)
    span = convolution_filter_taps.shape[0]
    rim = from_behind(gated[tok_rows - (span - 1) :], "sp", 1)
    padded = jnp.concatenate([rim, gated], axis=0)
    filtered = jnp.zeros(gated.shape, jnp.float32)
    for offset in range(span):
        filtered = filtered + convolution_filter_taps[offset] * padded[offset : offset + tok_rows]
    total_sum, total_square = lax.psum(
        (jnp.sum(filtered, axis=-1), jnp.sum(filtered * filtered, axis=-1)), "tp"
    )
    conv_channels = filtered.shape[1] * lax.axis_size("tp")
    row_mean = total_sum / conv_channels
    deviation = filtered - row_mean[:, None]
    variance = total_square / conv_channels - row_mean * row_mean
    conv_mixed = jax.nn.silu(
        deviation * lax.rsqrt(variance + LAYER_EPSILON)[:, None] * convolution_channel_gain
    ).astype(jnp.bfloat16)
    contract_dims = (((1,), (1,)), ((), ()))
    pieces = lax.all_gather(
        (attention_output_matrix, convolution_output_matrix), "sp", axis=0, tiled=True
    )
    partial_out = lax.dot_general(
        state_mixed, pieces[0], contract_dims, preferred_element_type=jnp.float32
    ) + lax.dot_general(conv_mixed, pieces[1], contract_dims, preferred_element_type=jnp.float32)
    return lax.psum(partial_out.astype(jnp.bfloat16), "tp")


def solution(mesh):
    return jax.shard_map(
        body,
        mesh=mesh,
        in_specs=(
            P("sp", None),
            P(),
            P("sp", "tp"),
            P("sp", "tp"),
            P("sp", "tp"),
            P("sp", "tp"),
            P("sp", "tp"),
            P("tp"),
            P(),
            P(None, "tp"),
            P("tp"),
            P(),
            P(None, "tp"),
            P("sp", "tp"),
            P("sp", "tp"),
            P("tp"),
            P(None, "tp"),
            P("tp"),
            P("sp", "tp"),
            P("sp", "tp"),
        ),
        out_specs=P("sp", None),
        check_vma=False,
    )
```

```python
import functools
import math

import jax
import jax.numpy as jnp
from jax import lax
from jax.experimental import pallas as pl
from jax.experimental.pallas import tpu as pltpu
from jax.sharding import PartitionSpec as P


MESH = pl.DeviceIdType.MESH
HIGHEST = lax.Precision.HIGHEST
RMS_EPSILON = 1e-06
GROUP_EPSILON = 0.00064
LAYER_EPSILON = 1e-05
UNIT_EPSILON = 1e-06
EXP_HALF = math.exp(-0.5)


def split(x):
    top = x.astype(jnp.bfloat16)
    return top, (x - top.astype(jnp.float32)).astype(jnp.bfloat16)


def dot3(left, right, dims=((1,), (0,))):
    (lh, ll), (rh, rl) = split(left), split(right)

    def one(p, q):
        return lax.dot_general(p, q, (dims, ((), ())), preferred_element_type=jnp.float32)

    return one(lh, rh) + (one(lh, rl) + one(ll, rh))


def dot3t(left, right):
    return dot3(left, right, ((1,), (1,)))


def exact(left, right):
    return jnp.dot(left, right, precision=HIGHEST, preferred_element_type=jnp.float32)


def column(values, index):
    lanes = lax.broadcasted_iota(jnp.int32, values.shape, 1)
    return jnp.sum(jnp.where(lanes == index, values, 0.0), axis=1, keepdims=True)


def delta_kernel(
    head_size, chunk, block,
    query_ref, key_ref, value_ref, decay_ref, rate_ref, factor_ref, share_ref,
    local_ref, carried_ref, pair_ref,
):
    rows, width = query_ref.shape
    pair = pl.program_id(0)
    per = width // head_size
    lane = lax.broadcasted_iota(jnp.int32, (1, width), 1)
    lane_head = lane // head_size
    row_w = lax.broadcasted_iota(jnp.int32, (width, width), 0)
    col_w = lax.broadcasted_iota(jnp.int32, (width, width), 1)
    same_head = (row_w // head_size) == (col_w // head_size)
    ones_head = jnp.where(same_head, 1.0, 0.0)
    row_b = lax.broadcasted_iota(jnp.int32, (block, block), 0)
    col_b = lax.broadcasted_iota(jnp.int32, (block, block), 1)
    same_chunk = (row_b // chunk) == (col_b // chunk)
    strict = same_chunk & (row_b > col_b)
    incl = same_chunk & (row_b >= col_b)
    sums = jnp.concatenate([jnp.where(incl, 1.0, 0.0), jnp.where(same_chunk, 1.0, 0.0)], axis=0)
    eye_b = jnp.where(row_b == col_b, 1.0, 0.0)

    factor, share = factor_ref[...], jnp.log(share_ref[...])
    factor_w = jnp.zeros((rows, width), jnp.float32)
    share_w = jnp.zeros((rows, width), jnp.float32)
    for h in range(per):
        factor_w = jnp.where(lane_head == h, column(factor, pair * per + h), factor_w)
        share_w = jnp.where(lane_head == h, column(share, pair * per + h), share_w)
    logdec = share_w - (EXP_HALF * jax.nn.sigmoid(decay_ref[...])) * factor_w
    learn = jax.nn.sigmoid(rate_ref[...])
    key = key_ref[...]
    unit = key * lax.rsqrt(exact(key * key, ones_head) + UNIT_EPSILON)

    blocks = []
    for start in range(0, rows, block):
        cut = slice(start, start + block)
        q, k, v, ld = query_ref[cut], key[cut], value_ref[cut], logdec[cut]
        er, wr = -unit[cut], unit[cut] * learn[cut]
        both = exact(sums, ld)
        gain, total = both[:block], both[block:]
        mid = 0.5 * total
        up, down, bup = jnp.exp(gain - mid), jnp.exp(mid - gain), jnp.exp(gain - ld - mid)
        ehat, qhat, what, khat = er * bup, q * up, wr * down, k * down
        right = jnp.concatenate([what, khat], axis=0)
        eh_full, q_full = er * jnp.exp(gain - ld), q * jnp.exp(gain)
        to_end = jnp.exp(total - gain)
        pulled = solved = local = query = None
        heads = []
        for h in range(per):
            left = jnp.where(lane_head == h, jnp.concatenate([ehat, qhat], axis=0), 0.0)
            grid = dot3t(left, right)
            ew = jnp.where(strict, grid[:block, :block], 0.0)
            ek = jnp.where(strict, grid[:block, block:], 0.0)
            rw = jnp.where(incl, grid[block:, :block], 0.0)
            rk = jnp.where(incl, grid[block:, block:], 0.0)
            size = 2
            off = (row_b // size == col_b // size) & (row_b > col_b)
            inv = eye_b + jnp.where(off, ew, 0.0)
            while size < chunk:
                off = (row_b // (2 * size) == col_b // (2 * size)) & (row_b // size > col_b // size)
                inv = inv + dot3(dot3(inv, jnp.where(off, ew, 0.0)), inv)
                size *= 2
            seen = dot3(jnp.concatenate([ek, rk], axis=0), v)
            both = dot3(inv, jnp.concatenate([seen[:block], eh_full], axis=1))
            read = dot3(rw, both)
            heads.append((both[:, :width], both[:, width:], read[:, :width] + seen[block:], read[:, width:]))
        merged = list(heads[0])
        for h in range(1, per):
            merged = [jnp.where(lane_head == h, new, old) for new, old in zip(heads[h], merged)]
        pulled, solved, local, query = merged
        blocks.append((pulled, solved, local, q_full + query, v, wr * to_end, k * to_end, jnp.exp(total)))

    state = jnp.concatenate([jnp.where(row_w == col_w, 1.0, 0.0), jnp.zeros((width, width), jnp.float32)], axis=0)
    across = ((0,), (0,))
    for number, (pulled, solved, local, query, v, wend, kend, gain) in enumerate(blocks):
        for first in range(0, block, chunk):
            cut = slice(first, first + chunk)
            place = slice(number * block + first, number * block + first + chunk)
            got = dot3t(query[cut], state)
            carried_ref[place] = got[:, :width]
            local_ref[place] = local[cut] + got[:, width:]
            step = jnp.where(same_head, dot3(solved[cut], wend[cut], across), 0.0)
            added = dot3(
                jnp.concatenate([pulled[cut], v[cut]], axis=0),
                jnp.concatenate([wend[cut], kend[cut]], axis=0),
                across,
            )
            added = jnp.where(same_head, added, 0.0)
            moved = state * gain[first : first + 1] + dot3(state, step)
            state = jnp.concatenate([moved[:width], moved[width:] + added], axis=0)
    pair_ref[0] = state


def finish_kernel(head_size, local_ref, carried_ref, state_ref, gain_ref, out_ref):
    width = local_ref.shape[1]
    row_w = lax.broadcasted_iota(jnp.int32, (width, width), 0)
    col_w = lax.broadcasted_iota(jnp.int32, (width, width), 1)
    same_head = (row_w // head_size) == (col_w // head_size)
    average = jnp.where(same_head, 1.0 / head_size, 0.0)
    y = local_ref[...] + dot3t(carried_ref[...], state_ref[0])
    centred = y - exact(y, average)
    variance = exact(centred * centred, average)
    out_ref[...] = (centred * lax.rsqrt(variance + GROUP_EPSILON) * gain_ref[...]).astype(jnp.bfloat16)


def from_behind(value, axis, steps):
    count = lax.axis_size(axis)
    initial, last = (max(0, -steps), min(count, count - steps))
    return lax.ppermute(value, axis, [(source, source + steps) for source in range(initial, last)])


def head_blocks(pairs, head_size):
    width = pairs.shape[-1]
    return jnp.stack(
        [pairs[:, a : a + head_size, a : a + head_size] for a in range(0, width, head_size)], axis=1
    )


def delta_rule(query, key, value, decay_pre, rate_pre, factor, share, gain):
    rows, channels = query.shape
    heads = factor.shape[1]
    head_size = channels // heads
    per = math.gcd(heads, max(1, 128 // head_size))
    width, pairs = per * head_size, heads // per
    block = math.gcd(rows, 128)
    chunk = math.gcd(block, 16)
    wide = pl.BlockSpec((rows, width), lambda i: (0, i))
    whole = pl.BlockSpec((rows, heads), lambda i: (0, 0))
    local, carried, pair = pl.pallas_call(
        functools.partial(delta_kernel, head_size, chunk, block),
        grid=(pairs,),
        in_specs=[wide] * 5 + [whole] * 2,
        out_specs=[wide, wide, pl.BlockSpec((1, 2 * width, width), lambda i: (i, 0, 0))],
        out_shape=[
            jax.ShapeDtypeStruct((rows, channels), jnp.float32),
            jax.ShapeDtypeStruct((rows, channels), jnp.float32),
            jax.ShapeDtypeStruct((pairs, 2 * width, width), jnp.float32),
        ],
        cost_estimate=pl.CostEstimate(
            flops=pairs * rows * width * width * 60, bytes_accessed=rows * channels * 32, transcendentals=rows * channels * 10
        ),
        name="delta_chunks",
    )(query, key, value, decay_pre, rate_pre, factor, share)

    phi, psi = head_blocks(pair[:, :width], head_size), head_blocks(pair[:, width:], head_size)
    both = jnp.concatenate([phi, psi], axis=-2).reshape(heads, 2 * head_size, head_size)
    count, place = lax.axis_size("sp"), lax.axis_index("sp")
    steps = 1
    while steps < count - 1:
        earlier = from_behind(both, "sp", steps)
        new = exact_mul("hcd,hde->hce", earlier, both[:, :head_size])
        new = new + jnp.concatenate([jnp.zeros_like(both[:, :head_size]), both[:, head_size:]], axis=1)
        both = jnp.where(place >= steps, new, both)
        steps *= 2
    state = from_behind(both[:, head_size:], "sp", 1).reshape(pairs, per, head_size, head_size)
    same = jnp.eye(per, dtype=jnp.float32)
    state = (state[:, :, :, None, :] * same[None, :, None, :, None]).reshape(pairs, width, width)
    return pl.pallas_call(
        functools.partial(finish_kernel, head_size),
        grid=(pairs,),
        in_specs=[wide, wide, pl.BlockSpec((1, width, width), lambda i: (i, 0, 0)), pl.BlockSpec((1, width), lambda i: (0, i))],
        out_specs=wide,
        out_shape=jax.ShapeDtypeStruct((rows, channels), jnp.bfloat16),
        name="delta_finish",
    )(local, carried, state, gain[None])


def exact_mul(form, left, right):
    return jnp.einsum(form, left, right, precision=HIGHEST)


def gather_kernel(axis, radices, number, *refs):
    ins, outs = refs[:number], refs[number : 2 * number]
    own_sem, far_send, far_recv, near_send, near_recv = refs[2 * number :]
    outer, middle, inner = radices
    me = lax.axis_index(axis)
    x, y, z = me % inner, (me // inner) % middle, me // (inner * middle)

    def index(z_at, y_at, x_at):
        return (z_at * middle + y_at) * inner + x_at

    far = [index((z + step) % outer, y, x) for step in range(1, outer)]
    near = {}
    if inner == 2:
        near["x"] = index(z, y, 1 - x)
    if middle == 2:
        near["y"] = index(z, 1 - y, x)
    barrier = pltpu.get_barrier_semaphore()
    peers = far + list(near.values())
    for peer in peers:
        pl.semaphore_signal(barrier, inc=1, device_id={axis: peer}, device_id_type=MESH)
    pl.semaphore_wait(barrier, len(peers))

    def far_copy(w, step, to, z_from):
        return pltpu.make_async_remote_copy(
            src_ref=ins[w],
            dst_ref=outs[w].at[z_from, y, x],
            send_sem=far_send.at[w, step],
            recv_sem=far_recv.at[w, step],
            device_id={axis: to},
            device_id_type=MESH,
        )

    own = [pltpu.make_async_copy(ins[w], outs[w].at[z, y, x], own_sem.at[w]) for w in range(number)]
    for w in range(number):
        own[w].start()
        for step in range(outer - 1):
            far_copy(w, step, far[step], z).start()

    def region(w, order, stage, from_y, from_x):
        if stage == 0:
            return outs[w].at[:, from_y, from_x]
        return outs[w].at[:, from_y] if order[0] == "x" else outs[w].at[:, :, from_x]

    def near_copy(w, order, stage, from_y, from_x):
        part = region(w, order, stage, from_y, from_x)
        return pltpu.make_async_remote_copy(
            src_ref=part,
            dst_ref=part,
            send_sem=near_send.at[w, stage],
            recv_sem=near_recv.at[w, stage],
            device_id={axis: near[order[stage]]},
            device_id_type=MESH,
        )

    def theirs(w, order, stage):
        from_y, from_x = (y, 1 - x) if order[stage] == "x" else (1 - y, x)
        return near_copy(w, order, stage, from_y, from_x)

    names = list(near)
    orders = [names if w % 2 == 0 else names[::-1] for w in range(number)]

    def advance(w, stage):
        if stage == 0:
            own[w].wait()
            for step in range(outer - 1):
                far_copy(w, step, far[step], (z + outer - step - 1) % outer).wait_recv()
        else:
            theirs(w, orders[w], stage - 1).wait_recv()
        if stage < len(names):
            near_copy(w, orders[w], stage, y, x).start()

    last = len(names)
    for tick in range(number + last):
        for stage in range(last, -1, -1):
            w = tick - stage
            if 0 <= w < number:
                advance(w, stage)
    for w in range(number):
        for step in range(outer - 1):
            far_copy(w, step, far[step], z).wait_send()
        for stage in range(last):
            near_copy(w, orders[w], stage, y, x).wait_send()


def gather_rows(arrays, axis):
    count, number = lax.axis_size(axis), len(arrays)
    inner = math.gcd(count, 2)
    middle = math.gcd(count // inner, 2)
    radices = (count // inner // middle, middle, inner)
    outs = pl.pallas_call(
        functools.partial(gather_kernel, axis, radices, number),
        in_specs=[pl.BlockSpec(memory_space=pltpu.VMEM)] * number,
        out_specs=[pl.BlockSpec(memory_space=pl.ANY)] * number,
        out_shape=[jax.ShapeDtypeStruct(radices + item.shape, item.dtype) for item in arrays],
        scratch_shapes=[
            pltpu.SemaphoreType.DMA((number,)),
            pltpu.SemaphoreType.DMA((number, max(1, radices[0] - 1))),
            pltpu.SemaphoreType.DMA((number, max(1, radices[0] - 1))),
            pltpu.SemaphoreType.DMA((number, 2)),
            pltpu.SemaphoreType.DMA((number, 2)),
        ],
        compiler_params=pltpu.CompilerParams(collective_id=0, has_side_effects=True),
        cost_estimate=pl.CostEstimate(
            flops=10**9, bytes_accessed=sum(item.size for item in arrays) * 2 * count, transcendentals=0
        ),
        name="gather_rows",
    )(*arrays)
    return [out.reshape((-1,) + item.shape[1:]) for out, item in zip(outs, arrays)]


def body(
    tokens,
    input_norm_gain,
    query_matrix,
    key_matrix,
    value_matrix,
    convolution_value_matrix,
    convolution_gate_matrix,
    decay_offset_channel,
    decay_first_matrix,
    decay_second_matrix,
    learning_rate_offset,
    learning_rate_first_matrix,
    learning_rate_second_matrix,
    forgetting_rate_factor,
    state_retention_share,
    per_head_norm_gain,
    convolution_filter_taps,
    convolution_channel_gain,
    attention_output_matrix,
    convolution_output_matrix,
):
    tok_rows = tokens.shape[0]
    widened = tokens.astype(jnp.float32)
    normed = (
        widened
        * lax.rsqrt(jnp.mean(widened * widened, axis=-1, keepdims=True) + RMS_EPSILON)
        * input_norm_gain
    ).astype(jnp.bfloat16)
    pieces = gather_rows(
        (query_matrix, key_matrix, convolution_value_matrix, value_matrix, convolution_gate_matrix), "sp"
    )
    query_proj, key_proj, conv_value, value_proj, conv_gate = tuple(
        (jnp.dot(normed, piece, preferred_element_type=jnp.float32) for piece in pieces)
    )
    decay_mid = jnp.tanh(
        jnp.dot(normed, decay_first_matrix, preferred_element_type=jnp.float32)
    ).astype(jnp.bfloat16)
    rate_mid = jnp.dot(
        normed, learning_rate_first_matrix, preferred_element_type=jnp.float32
    ).astype(jnp.bfloat16)
    decay_pre = decay_offset_channel + jnp.dot(
        decay_mid, decay_second_matrix, preferred_element_type=jnp.float32
    )
    rate_pre = learning_rate_offset + jnp.dot(
        rate_mid, learning_rate_second_matrix, preferred_element_type=jnp.float32
    )
    state_mixed = delta_rule(
        query_proj, key_proj, value_proj, decay_pre, rate_pre,
        forgetting_rate_factor, state_retention_share, per_head_norm_gain,
    )
    gated = (conv_value * jax.nn.sigmoid(conv_gate)).astype(jnp.bfloat16)
    span = convolution_filter_taps.shape[0]
    rim = from_behind(gated[tok_rows - (span - 1) :], "sp", 1)
    padded = jnp.concatenate([rim, gated], axis=0)
    filtered = jnp.zeros(gated.shape, jnp.float32)
    for offset in range(span):
        filtered = filtered + convolution_filter_taps[offset] * padded[offset : offset + tok_rows]
    total_sum, total_square = lax.psum(
        (jnp.sum(filtered, axis=-1), jnp.sum(filtered * filtered, axis=-1)), "tp"
    )
    conv_channels = filtered.shape[1] * lax.axis_size("tp")
    row_mean = total_sum / conv_channels
    deviation = filtered - row_mean[:, None]
    variance = total_square / conv_channels - row_mean * row_mean
    conv_mixed = jax.nn.silu(
        deviation * lax.rsqrt(variance + LAYER_EPSILON)[:, None] * convolution_channel_gain
    ).astype(jnp.bfloat16)
    contract_dims = (((1,), (1,)), ((), ()))
    pieces = lax.all_gather(
        (attention_output_matrix, convolution_output_matrix), "sp", axis=0, tiled=True
    )
    partial_out = lax.dot_general(
        state_mixed, pieces[0], contract_dims, preferred_element_type=jnp.float32
    ) + lax.dot_general(conv_mixed, pieces[1], contract_dims, preferred_element_type=jnp.float32)
    partial_out = partial_out.astype(jnp.bfloat16)
    if lax.axis_size("tp") != 2:
        return lax.psum(partial_out, "tp")
    other = lax.ppermute(partial_out, "tp", [(0, 1), (1, 0)])
    return (partial_out.astype(jnp.float32) + other.astype(jnp.float32)).astype(jnp.bfloat16)


def solution(mesh):
    return jax.shard_map(
        body,
        mesh=mesh,
        in_specs=(
            P("sp", None),
            P(),
            P("sp", "tp"),
            P("sp", "tp"),
            P("sp", "tp"),
            P("sp", "tp"),
            P("sp", "tp"),
            P("tp"),
            P(),
            P(None, "tp"),
            P("tp"),
            P(),
            P(None, "tp"),
            P("sp", "tp"),
            P("sp", "tp"),
            P("tp"),
            P(None, "tp"),
            P("tp"),
            P("sp", "tp"),
            P("sp", "tp"),
        ),
        out_specs=P("sp", None),
        check_vma=False,
    )
```

```python
import functools
import math

import jax
import jax.numpy as jnp
from jax import lax
from jax.experimental import pallas as pl
from jax.experimental.pallas import tpu as pltpu
from jax.sharding import PartitionSpec as P


MESH = pl.DeviceIdType.MESH
HIGHEST = lax.Precision.HIGHEST
RMS_EPSILON = 1e-06
GROUP_EPSILON = 0.00064
LAYER_EPSILON = 1e-05
UNIT_EPSILON = 1e-06
EXP_HALF = math.exp(-0.5)


def split(x):
    top = x.astype(jnp.bfloat16)
    return top, (x - top.astype(jnp.float32)).astype(jnp.bfloat16)


def dot3(left, right, dims=((1,), (0,))):
    (lh, ll), (rh, rl) = split(left), split(right)

    def one(p, q):
        return lax.dot_general(p, q, (dims, ((), ())), preferred_element_type=jnp.float32)

    return one(lh, rh) + (one(lh, rl) + one(ll, rh))


def dot3t(left, right):
    return dot3(left, right, ((1,), (1,)))


def exact(left, right):
    return jnp.dot(left, right, precision=HIGHEST, preferred_element_type=jnp.float32)


def column(values, index):
    lanes = lax.broadcasted_iota(jnp.int32, values.shape, 1)
    return jnp.sum(jnp.where(lanes == index, values, 0.0), axis=1, keepdims=True)


def delta_kernel(
    head_size, chunk, block,
    query_ref, key_ref, value_ref, decay_ref, rate_ref, factor_ref, share_ref,
    local_ref, carried_ref, pair_ref,
):
    rows, width = query_ref.shape
    pair = pl.program_id(0)
    per = width // head_size
    lane = lax.broadcasted_iota(jnp.int32, (1, width), 1)
    lane_head = lane // head_size
    row_w = lax.broadcasted_iota(jnp.int32, (width, width), 0)
    col_w = lax.broadcasted_iota(jnp.int32, (width, width), 1)
    same_head = (row_w // head_size) == (col_w // head_size)
    ones_head = jnp.where(same_head, 1.0, 0.0)
    row_b = lax.broadcasted_iota(jnp.int32, (block, block), 0)
    col_b = lax.broadcasted_iota(jnp.int32, (block, block), 1)
    same_chunk = (row_b // chunk) == (col_b // chunk)
    strict = same_chunk & (row_b > col_b)
    incl = same_chunk & (row_b >= col_b)
    sums = jnp.concatenate([jnp.where(incl, 1.0, 0.0), jnp.where(same_chunk, 1.0, 0.0)], axis=0)
    eye_b = jnp.where(row_b == col_b, 1.0, 0.0)

    factor, share = factor_ref[...], jnp.log(share_ref[...])
    factor_w = jnp.zeros((rows, width), jnp.float32)
    share_w = jnp.zeros((rows, width), jnp.float32)
    for h in range(per):
        factor_w = jnp.where(lane_head == h, column(factor, pair * per + h), factor_w)
        share_w = jnp.where(lane_head == h, column(share, pair * per + h), share_w)
    logdec = share_w - (EXP_HALF * jax.nn.sigmoid(decay_ref[...])) * factor_w
    learn = jax.nn.sigmoid(rate_ref[...])
    key = key_ref[...]
    unit = key * lax.rsqrt(exact(key * key, ones_head) + UNIT_EPSILON)

    blocks = []
    for start in range(0, rows, block):
        cut = slice(start, start + block)
        q, k, v, ld = query_ref[cut], key[cut], value_ref[cut], logdec[cut]
        er, wr = -unit[cut], unit[cut] * learn[cut]
        both = exact(sums, ld)
        gain, total = both[:block], both[block:]
        mid = 0.5 * total
        up, down, bup = jnp.exp(gain - mid), jnp.exp(mid - gain), jnp.exp(gain - ld - mid)
        ehat, qhat, what, khat = er * bup, q * up, wr * down, k * down
        right = jnp.concatenate([what, khat], axis=0)
        eh_full, q_full = er * jnp.exp(gain - ld), q * jnp.exp(gain)
        to_end = jnp.exp(total - gain)
        pulled = solved = local = query = None
        heads = []
        for h in range(per):
            left = jnp.where(lane_head == h, jnp.concatenate([ehat, qhat], axis=0), 0.0)
            grid = dot3t(left, right)
            ew = jnp.where(strict, grid[:block, :block], 0.0)
            ek = jnp.where(strict, grid[:block, block:], 0.0)
            rw = jnp.where(incl, grid[block:, :block], 0.0)
            rk = jnp.where(incl, grid[block:, block:], 0.0)
            size = 2
            off = (row_b // size == col_b // size) & (row_b > col_b)
            inv = eye_b + jnp.where(off, ew, 0.0)
            while size < chunk:
                off = (row_b // (2 * size) == col_b // (2 * size)) & (row_b // size > col_b // size)
                inv = inv + dot3(dot3(inv, jnp.where(off, ew, 0.0)), inv)
                size *= 2
            seen = dot3(jnp.concatenate([ek, rk], axis=0), v)
            both = dot3(inv, jnp.concatenate([seen[:block], eh_full], axis=1))
            read = dot3(rw, both)
            heads.append((both[:, :width], both[:, width:], read[:, :width] + seen[block:], read[:, width:]))
        merged = list(heads[0])
        for h in range(1, per):
            merged = [jnp.where(lane_head == h, new, old) for new, old in zip(heads[h], merged)]
        pulled, solved, local, query = merged
        blocks.append((pulled, solved, local, q_full + query, v, wr * to_end, k * to_end, jnp.exp(total)))

    state = jnp.concatenate([jnp.where(row_w == col_w, 1.0, 0.0), jnp.zeros((width, width), jnp.float32)], axis=0)
    across = ((0,), (0,))
    for number, (pulled, solved, local, query, v, wend, kend, gain) in enumerate(blocks):
        for first in range(0, block, chunk):
            cut = slice(first, first + chunk)
            place = slice(number * block + first, number * block + first + chunk)
            got = dot3t(query[cut], state)
            carried_ref[place] = got[:, :width]
            local_ref[place] = local[cut] + got[:, width:]
            step = jnp.where(same_head, dot3(solved[cut], wend[cut], across), 0.0)
            added = dot3(
                jnp.concatenate([pulled[cut], v[cut]], axis=0),
                jnp.concatenate([wend[cut], kend[cut]], axis=0),
                across,
            )
            added = jnp.where(same_head, added, 0.0)
            moved = state * gain[first : first + 1] + dot3(state, step)
            state = jnp.concatenate([moved[:width], moved[width:] + added], axis=0)
    pair_ref[0] = state


def finish_kernel(head_size, local_ref, carried_ref, state_ref, gain_ref, out_ref):
    width = local_ref.shape[1]
    row_w = lax.broadcasted_iota(jnp.int32, (width, width), 0)
    col_w = lax.broadcasted_iota(jnp.int32, (width, width), 1)
    same_head = (row_w // head_size) == (col_w // head_size)
    average = jnp.where(same_head, 1.0 / head_size, 0.0)
    y = local_ref[...] + dot3t(carried_ref[...], state_ref[0])
    centred = y - exact(y, average)
    variance = exact(centred * centred, average)
    out_ref[...] = (centred * lax.rsqrt(variance + GROUP_EPSILON) * gain_ref[...]).astype(jnp.bfloat16)


def from_behind(value, axis, steps):
    count = lax.axis_size(axis)
    initial, last = (max(0, -steps), min(count, count - steps))
    return lax.ppermute(value, axis, [(source, source + steps) for source in range(initial, last)])


def head_blocks(pairs, head_size):
    width = pairs.shape[-1]
    return jnp.stack(
        [pairs[:, a : a + head_size, a : a + head_size] for a in range(0, width, head_size)], axis=1
    )


def delta_rule(query, key, value, decay_pre, rate_pre, factor, share, gain):
    rows, channels = query.shape
    heads = factor.shape[1]
    head_size = channels // heads
    per = math.gcd(heads, max(1, 128 // head_size))
    width, pairs = per * head_size, heads // per
    block = math.gcd(rows, 128)
    chunk = math.gcd(block, 16)
    wide = pl.BlockSpec((rows, width), lambda i: (0, i))
    whole = pl.BlockSpec((rows, heads), lambda i: (0, 0))
    local, carried, pair = pl.pallas_call(
        functools.partial(delta_kernel, head_size, chunk, block),
        grid=(pairs,),
        in_specs=[wide] * 5 + [whole] * 2,
        out_specs=[wide, wide, pl.BlockSpec((1, 2 * width, width), lambda i: (i, 0, 0))],
        out_shape=[
            jax.ShapeDtypeStruct((rows, channels), jnp.float32),
            jax.ShapeDtypeStruct((rows, channels), jnp.float32),
            jax.ShapeDtypeStruct((pairs, 2 * width, width), jnp.float32),
        ],
        cost_estimate=pl.CostEstimate(
            flops=pairs * rows * width * width * 60, bytes_accessed=rows * channels * 32, transcendentals=rows * channels * 10
        ),
        name="delta_chunks",
    )(query, key, value, decay_pre, rate_pre, factor, share)

    phi, psi = head_blocks(pair[:, :width], head_size), head_blocks(pair[:, width:], head_size)
    both = jnp.concatenate([phi, psi], axis=-2).reshape(heads, 2 * head_size, head_size)
    count, place = lax.axis_size("sp"), lax.axis_index("sp")
    steps = 1
    while steps < count - 1:
        earlier = from_behind(both, "sp", steps)
        new = exact_mul("hcd,hde->hce", earlier, both[:, :head_size])
        new = new + jnp.concatenate([jnp.zeros_like(both[:, :head_size]), both[:, head_size:]], axis=1)
        both = jnp.where(place >= steps, new, both)
        steps *= 2
    state = from_behind(both[:, head_size:], "sp", 1).reshape(pairs, per, head_size, head_size)
    same = jnp.eye(per, dtype=jnp.float32)
    state = (state[:, :, :, None, :] * same[None, :, None, :, None]).reshape(pairs, width, width)
    return pl.pallas_call(
        functools.partial(finish_kernel, head_size),
        grid=(pairs,),
        in_specs=[wide, wide, pl.BlockSpec((1, width, width), lambda i: (i, 0, 0)), pl.BlockSpec((1, width), lambda i: (0, i))],
        out_specs=wide,
        out_shape=jax.ShapeDtypeStruct((rows, channels), jnp.bfloat16),
        name="delta_finish",
    )(local, carried, state, gain[None])


def exact_mul(form, left, right):
    return jnp.einsum(form, left, right, precision=HIGHEST)


def gather_kernel(axis, radices, number, *refs):
    ins, outs = refs[:number], refs[number : 2 * number]
    own_sem, far_send, far_recv, near_send, near_recv = refs[2 * number :]
    outer, middle, inner = radices
    me = lax.axis_index(axis)
    x, y, z = me % inner, (me // inner) % middle, me // (inner * middle)

    def index(z_at, y_at, x_at):
        return (z_at * middle + y_at) * inner + x_at

    far = [index((z + step) % outer, y, x) for step in range(1, outer)]
    near = {}
    if inner == 2:
        near["x"] = index(z, y, 1 - x)
    if middle == 2:
        near["y"] = index(z, 1 - y, x)
    barrier = pltpu.get_barrier_semaphore()
    peers = far + list(near.values())
    for peer in peers:
        pl.semaphore_signal(barrier, inc=1, device_id={axis: peer}, device_id_type=MESH)
    pl.semaphore_wait(barrier, len(peers))

    def far_copy(w, step, to, z_from):
        return pltpu.make_async_remote_copy(
            src_ref=ins[w],
            dst_ref=outs[w].at[z_from, y, x],
            send_sem=far_send.at[w, step],
            recv_sem=far_recv.at[w, step],
            device_id={axis: to},
            device_id_type=MESH,
        )

    own = [pltpu.make_async_copy(ins[w], outs[w].at[z, y, x], own_sem.at[w]) for w in range(number)]
    for w in range(number):
        own[w].start()
        for step in range(outer - 1):
            far_copy(w, step, far[step], z).start()

    def region(w, order, stage, from_y, from_x):
        if stage == 0:
            return outs[w].at[:, from_y, from_x]
        return outs[w].at[:, from_y] if order[0] == "x" else outs[w].at[:, :, from_x]

    def near_copy(w, order, stage, from_y, from_x):
        part = region(w, order, stage, from_y, from_x)
        return pltpu.make_async_remote_copy(
            src_ref=part,
            dst_ref=part,
            send_sem=near_send.at[w, stage],
            recv_sem=near_recv.at[w, stage],
            device_id={axis: near[order[stage]]},
            device_id_type=MESH,
        )

    def theirs(w, order, stage):
        from_y, from_x = (y, 1 - x) if order[stage] == "x" else (1 - y, x)
        return near_copy(w, order, stage, from_y, from_x)

    names = list(near)
    orders = [names if w % 2 == 0 else names[::-1] for w in range(number)]

    def advance(w, stage):
        if stage == 0:
            own[w].wait()
            for step in range(outer - 1):
                far_copy(w, step, far[step], (z + outer - step - 1) % outer).wait_recv()
        else:
            theirs(w, orders[w], stage - 1).wait_recv()
        if stage < len(names):
            near_copy(w, orders[w], stage, y, x).start()

    last = len(names)
    for tick in range(number + last):
        for stage in range(last, -1, -1):
            w = tick - stage
            if 0 <= w < number:
                advance(w, stage)
    for w in range(number):
        for step in range(outer - 1):
            far_copy(w, step, far[step], z).wait_send()
        for stage in range(last):
            near_copy(w, orders[w], stage, y, x).wait_send()


def gather_rows(arrays, axis):
    count, number = lax.axis_size(axis), len(arrays)
    inner = math.gcd(count, 2)
    middle = math.gcd(count // inner, 2)
    radices = (count // inner // middle, middle, inner)
    outs = pl.pallas_call(
        functools.partial(gather_kernel, axis, radices, number),
        in_specs=[pl.BlockSpec(memory_space=pltpu.VMEM)] * number,
        out_specs=[pl.BlockSpec(memory_space=pl.ANY)] * number,
        out_shape=[jax.ShapeDtypeStruct(radices + item.shape, item.dtype) for item in arrays],
        scratch_shapes=[
            pltpu.SemaphoreType.DMA((number,)),
            pltpu.SemaphoreType.DMA((number, max(1, radices[0] - 1))),
            pltpu.SemaphoreType.DMA((number, max(1, radices[0] - 1))),
            pltpu.SemaphoreType.DMA((number, 2)),
            pltpu.SemaphoreType.DMA((number, 2)),
        ],
        compiler_params=pltpu.CompilerParams(collective_id=0, has_side_effects=True),
        cost_estimate=pl.CostEstimate(
            flops=10**9, bytes_accessed=sum(item.size for item in arrays) * 2 * count, transcendentals=0
        ),
        name="gather_rows",
    )(*arrays)
    return [out.reshape((-1,) + item.shape[1:]) for out, item in zip(outs, arrays)]


def body(
    tokens,
    input_norm_gain,
    query_matrix,
    key_matrix,
    value_matrix,
    convolution_value_matrix,
    convolution_gate_matrix,
    decay_offset_channel,
    decay_first_matrix,
    decay_second_matrix,
    learning_rate_offset,
    learning_rate_first_matrix,
    learning_rate_second_matrix,
    forgetting_rate_factor,
    state_retention_share,
    per_head_norm_gain,
    convolution_filter_taps,
    convolution_channel_gain,
    attention_output_matrix,
    convolution_output_matrix,
):
    tok_rows = tokens.shape[0]
    widened = tokens.astype(jnp.float32)
    normed = (
        widened
        * lax.rsqrt(jnp.mean(widened * widened, axis=-1, keepdims=True) + RMS_EPSILON)
        * input_norm_gain
    ).astype(jnp.bfloat16)
    pieces = (
        *gather_rows((query_matrix, key_matrix, value_matrix), "sp"),
        lax.all_gather(convolution_value_matrix, "sp", axis=0, tiled=True),
        lax.all_gather(convolution_gate_matrix, "sp", axis=0, tiled=True),
    )
    query_proj, key_proj, value_proj, conv_value, conv_gate = tuple(
        (jnp.dot(normed, piece, preferred_element_type=jnp.float32) for piece in pieces)
    )
    decay_mid = jnp.tanh(
        jnp.dot(normed, decay_first_matrix, preferred_element_type=jnp.float32)
    ).astype(jnp.bfloat16)
    rate_mid = jnp.dot(
        normed, learning_rate_first_matrix, preferred_element_type=jnp.float32
    ).astype(jnp.bfloat16)
    decay_pre = decay_offset_channel + jnp.dot(
        decay_mid, decay_second_matrix, preferred_element_type=jnp.float32
    )
    rate_pre = learning_rate_offset + jnp.dot(
        rate_mid, learning_rate_second_matrix, preferred_element_type=jnp.float32
    )
    state_mixed = delta_rule(
        query_proj, key_proj, value_proj, decay_pre, rate_pre,
        forgetting_rate_factor, state_retention_share, per_head_norm_gain,
    )
    gated = (conv_value * jax.nn.sigmoid(conv_gate)).astype(jnp.bfloat16)
    span = convolution_filter_taps.shape[0]
    rim = from_behind(gated[tok_rows - (span - 1) :], "sp", 1)
    padded = jnp.concatenate([rim, gated], axis=0)
    filtered = jnp.zeros(gated.shape, jnp.float32)
    for offset in range(span):
        filtered = filtered + convolution_filter_taps[offset] * padded[offset : offset + tok_rows]
    total_sum, total_square = lax.psum(
        (jnp.sum(filtered, axis=-1), jnp.sum(filtered * filtered, axis=-1)), "tp"
    )
    conv_channels = filtered.shape[1] * lax.axis_size("tp")
    row_mean = total_sum / conv_channels
    deviation = filtered - row_mean[:, None]
    variance = total_square / conv_channels - row_mean * row_mean
    conv_mixed = jax.nn.silu(
        deviation * lax.rsqrt(variance + LAYER_EPSILON)[:, None] * convolution_channel_gain
    ).astype(jnp.bfloat16)
    contract_dims = (((1,), (1,)), ((), ()))
    pieces = lax.all_gather(
        (attention_output_matrix, convolution_output_matrix), "sp", axis=0, tiled=True
    )
    partial_out = lax.dot_general(
        state_mixed, pieces[0], contract_dims, preferred_element_type=jnp.float32
    ) + lax.dot_general(conv_mixed, pieces[1], contract_dims, preferred_element_type=jnp.float32)
    partial_out = partial_out.astype(jnp.bfloat16)
    if lax.axis_size("tp") != 2:
        return lax.psum(partial_out, "tp")
    other = lax.ppermute(partial_out, "tp", [(0, 1), (1, 0)])
    return (partial_out.astype(jnp.float32) + other.astype(jnp.float32)).astype(jnp.bfloat16)


def solution(mesh):
    return jax.shard_map(
        body,
        mesh=mesh,
        in_specs=(
            P("sp", None),
            P(),
            P("sp", "tp"),
            P("sp", "tp"),
            P("sp", "tp"),
            P("sp", "tp"),
            P("sp", "tp"),
            P("tp"),
            P(),
            P(None, "tp"),
            P("tp"),
            P(),
            P(None, "tp"),
            P("sp", "tp"),
            P("sp", "tp"),
            P("tp"),
            P(None, "tp"),
            P("tp"),
            P("sp", "tp"),
            P("sp", "tp"),
        ),
        out_specs=P("sp", None),
        check_vma=False,
    )
```
